32 devices in a mesh: sp: 8 (over z, y), tp: 4 (over x, core).
Axes of the slice: x: 2, y: 2, z: 4, core: 2. Of those that a mesh axis runs over, the one named last changes fastest.
Arguments:
- tokens: bfloat16 [2560, 2048], P('sp', 'tp'), may hold values from -6 to 6
- pre_gain: float32 [2, 2048], replicated, may hold values from 0.1 to 1.9
- w_value: bfloat16 [2, 2048, 2048], P(None, 'sp', 'tp'), may hold values from -0.125 to 0.125
- w_gate: bfloat16 [2, 2048, 2048], P(None, 'sp', 'tp'), may hold values from -0.125 to 0.125
- taps: float32 [2, 31, 2048], P(None, None, 'tp'), may hold values from -5 to 5
- norm_gain: float32 [2, 2048], P(None, 'tp'), may hold values from 0.1 to 1.9
- norm_shift: float32 [2, 2048], P(None, 'tp'), may hold values from -3 to 3
- w_out: bfloat16 [2, 2048, 2048], P(None, 'tp', 'sp'), may hold values from -2 to 2
- post_gain: float32 [2, 2048], P(None, 'tp'), may hold values from 0.1 to 1.9
Outputs:
- stream: bfloat16 [2560, 2048], P('sp', 'tp')
The draws below stay inside these ranges and needn't reach their ends.
All inputs are finite; a program needn't handle non-finite values.
Results may differ from the reference program's by a relative error of at most 0.015.
Values may be sent and summed in bfloat16 or wider, within the bound.
A program may use at most 64 MiB of HBM per device.

```python
import jax
import jax.numpy as jnp
from jax import lax

D = 2048
CONV_WIDTH = 31
LAYERS = 2
TOKENS = 2560
N_TP = 4


def draw_taps(key, part):
    first, second, third = jax.random.split(jax.random.fold_in(key, 7), 3)
    base = jax.random.truncated_normal(first, -4.0, 4.0, (LAYERS, CONV_WIDTH, D), jnp.float32) * CONV_WIDTH ** (-0.5)
    channel = jnp.exp(jax.random.uniform(second, (LAYERS, 1, D), jnp.float32, -0.7, 0.7))
    levels = jnp.array([0.4, 0.8, 1.6, 3.2], jnp.float32)
    order = jnp.stack([jax.random.permutation(jax.random.fold_in(third, layer), 4) for layer in range(LAYERS)])
    groups = jnp.repeat(levels[order], D // 4, axis=1)
    return base * channel * groups[:, None, :]


def draw_w_out(key, part):
    first, second = jax.random.split(jax.random.fold_in(key, 11), 2)
    base = jax.random.truncated_normal(first, -4.0, 4.0, (LAYERS, D, D), jnp.float32) * D ** (-0.5)
    levels = jnp.array([0.4, 0.8, 1.6, 3.2], jnp.float32)
    order = jnp.stack([jax.random.permutation(jax.random.fold_in(second, layer), 4) for layer in range(LAYERS)])
    groups = jnp.repeat(levels[order], D // 4, axis=1)
    return (base * groups[:, None, :]).astype(jnp.bfloat16)


def shard_levels(own_key, shape, shards, low, largest):
    loudness = 1.0
    for position, parts in shards:
        draws = jax.random.uniform(jax.random.fold_in(jax.random.fold_in(own_key, 6), position), (parts,), jnp.float32, low / len(shards), largest / len(shards))
        loudness = loudness * jnp.repeat(jnp.exp(draws), shape[position] // parts).reshape((-1,) + (1,) * (len(shape) - 1 - position))
    return loudness


def noise(rng, shape, width, most, pieces=(), dtype=jnp.bfloat16):
    values = jax.random.normal(rng, shape, jnp.float32) * width
    if len(pieces) > 0:
        values = shard_levels(rng, shape, pieces, -0.22, 0.18) * values
    return jnp.clip(values, min=-most, max=most).astype(dtype)


def setup_inputs(seed: int = 0) -> dict:
    keys = jax.random.split(jax.random.key(seed), 10)
    tokens = noise(keys[0], (TOKENS, D), 1.0, 6.0, ((0, 8), (1, 4)))
    pre_gain = jnp.clip(1.0 + 0.18 * jax.random.normal(keys[1], (LAYERS, D), jnp.float32), 0.1, 1.9)
    w_value = noise(keys[2], (LAYERS, D, D), D ** -0.5, 0.125, ((1, 8), (2, 4)))
    w_gate = noise(keys[3], (LAYERS, D, D), D ** -0.5, 0.125, ((1, 8), (2, 4)))
    taps = draw_taps(jax.random.fold_in(keys[9], 71), 0)
    norm_gain = jnp.clip(1.0 + 0.18 * jax.random.normal(keys[5], (LAYERS, D), jnp.float32), 0.1, 1.9)
    norm_shift = noise(keys[6], (LAYERS, D), 0.5, 3.0, ((1, 4),), jnp.float32)
    w_out = draw_w_out(jax.random.fold_in(keys[9], 71), 0)
    post_gain = jnp.clip(1.0 + 0.18 * jax.random.normal(keys[8], (LAYERS, D), jnp.float32), 0.1, 1.9)
    return dict(tokens=tokens, pre_gain=pre_gain, w_value=w_value, w_gate=w_gate, taps=taps, norm_gain=norm_gain, norm_shift=norm_shift, w_out=w_out, post_gain=post_gain)


EPSILON = 1e-06
LN_EPSILON = 1e-05

def reference(tokens, pre_gain, w_value, w_gate, taps, norm_gain, norm_shift, w_out, post_gain):
    stream = tokens
    block = D // N_TP
    for layer in range(LAYERS):
        stream_f = stream.astype(jnp.float32)
        normed = (stream_f * lax.rsqrt(lax.optimization_barrier(jnp.mean(stream_f * stream_f, -1, keepdims=True)) + EPSILON) * pre_gain[layer]).astype(jnp.bfloat16)
        value_proj = jnp.dot(normed, w_value[layer], preferred_element_type=jnp.float32)
        gate_proj = jnp.dot(normed, w_gate[layer], preferred_element_type=jnp.float32)
        glu_act = (value_proj * jax.nn.sigmoid(gate_proj)).astype(jnp.bfloat16)
        padded = jnp.pad(glu_act.astype(jnp.float32), ((CONV_WIDTH - 1, 0), (0, 0)))
        conv_out = jnp.zeros((TOKENS, D), jnp.float32)
        for offset in range(CONV_WIDTH):
            conv_out = conv_out + taps[layer, offset] * padded[offset:offset + TOKENS]
        center = lax.optimization_barrier(jnp.sum(conv_out, -1, keepdims=True)) / D
        spread = jnp.maximum(lax.optimization_barrier(jnp.sum(conv_out * conv_out, -1, keepdims=True)) / D - center * center, 0.0)
        activated = jax.nn.silu((conv_out - center) * lax.rsqrt(spread + LN_EPSILON) * norm_gain[layer] + norm_shift[layer]).astype(jnp.bfloat16)
        summed = jnp.zeros((TOKENS, D), jnp.float32)
        for start in range(0, D, block):
            partial_sum = jnp.dot(activated[:, start:start + block], w_out[layer, start:start + block, :], preferred_element_type=jnp.float32).astype(jnp.bfloat16)
            partial_sum = lax.optimization_barrier(partial_sum)
            summed = summed + partial_sum.astype(jnp.float32)
        projected = summed.astype(jnp.bfloat16).astype(jnp.float32)
        scale = lax.rsqrt(lax.optimization_barrier(jnp.mean(projected * projected, -1, keepdims=True)) + EPSILON)
        stream = (stream_f + projected * scale * post_gain[layer]).astype(jnp.bfloat16)
    return stream
```

```python
import functools

import jax
import jax.numpy as jnp
from jax import lax
from jax.experimental import pallas as pl
from jax.experimental.pallas import tpu as pltpu
from jax.sharding import PartitionSpec as P

D = 2048
CONV_WIDTH = 31
LAYERS = 2


EPSILON = 1e-06
LN_EPSILON = 1e-05


def passed_along(block, axis, distance):
    devices = range(lax.axis_size(axis))
    route = [(i - distance, i) for i in devices if i - distance in devices]
    return lax.ppermute(block, axis, route)


def local(tokens, pre_gain, w_value, w_gate, taps, norm_gain, norm_shift, w_out, post_gain):
    stream = tokens
    full_value, full_gate = (
        lax.all_gather(w_value, "sp", axis=1, tiled=True),
        lax.all_gather(w_gate, "sp", axis=1, tiled=True),
    )
    full_out = lax.all_gather(w_out, "sp", axis=2, tiled=True)
    for layer in range(LAYERS):
        whole = lax.all_gather(stream, "tp", axis=1, tiled=True)
        whole_f = whole.astype(jnp.float32)
        normed = (
            whole_f
            * lax.rsqrt(jnp.mean(whole_f * whole_f, -1, keepdims=True) + EPSILON)
            * pre_gain[layer]
        ).astype(jnp.bfloat16)
        value_mat = full_value[layer]
        gate_mat = full_gate[layer]
        out_mat = full_out[layer]
        value_proj = jnp.dot(normed, value_mat, preferred_element_type=jnp.float32)
        gate_proj = jnp.dot(normed, gate_mat, preferred_element_type=jnp.float32)
        glu_act = (value_proj * jax.nn.sigmoid(gate_proj)).astype(jnp.bfloat16)
        rows = glu_act.shape[0]
        fringe = passed_along(glu_act[rows - (CONV_WIDTH - 1) :], "sp", 1)
        padded = jnp.concatenate([fringe, glu_act], 0).astype(jnp.float32)
        conv_out = jnp.zeros(glu_act.shape, jnp.float32)
        for offset in range(CONV_WIDTH):
            conv_out = conv_out + taps[layer, offset] * padded[offset : offset + rows]
        row_sum, row_square = lax.psum(
            (jnp.sum(conv_out, -1, keepdims=True), jnp.sum(conv_out * conv_out, -1, keepdims=True)),
            "tp",
        )
        center = row_sum / D
        spread = jnp.maximum(row_square / D - center * center, 0.0)
        activated = jax.nn.silu(
            (conv_out - center) * lax.rsqrt(spread + LN_EPSILON) * norm_gain[layer]
            + norm_shift[layer]
        ).astype(jnp.bfloat16)
        terms = jnp.dot(activated, out_mat, preferred_element_type=jnp.float32)
        summed = lax.psum_scatter(terms.astype(jnp.bfloat16), "tp", scatter_dimension=1, tiled=True)
        projected = summed.astype(jnp.float32)
        out_square = lax.psum(jnp.sum(projected * projected, -1, keepdims=True), "tp")
        scale = lax.rsqrt(out_square / D + EPSILON)
        stream = (stream.astype(jnp.float32) + projected * scale * post_gain[layer]).astype(
            jnp.bfloat16
        )
    return stream


TILE = 64
HALO = 32
TWICE = (2,)


def step(
    nz, x_ref, pre_ref, wv_hbm, wg_hbm, taps_ref, ng_ref, ns_ref, wo_hbm, post_ref, out_ref,
    wvg, wo, whole, normed, glu, conv, act, part_out, part_in, cross_out, cross_in, total,
    stat, stat_in, local_sem, su, ru, sd, rd, ys, yr, gs, gr, hs, hr, ss, sr, ps, pr, cs, cr,
):
    sp, tp = lax.axis_index("sp"), lax.axis_index("tp")
    nsp, ntp = 2 * nz, 4
    z, y = sp // 2, sp % 2
    x, c = tp // 2, tp % 2
    up, down, beside = (sp + 2, tp), (sp - 2, tp), (z * 2 + 1 - y, tp)
    mate, across, diagonal = (sp, x * 2 + 1 - c), (sp, (1 - x) * 2 + c), (sp, (1 - x) * 2 + 1 - c)
    rows, cols = x_ref.shape
    layers = pre_ref.shape[0]
    units = 3 * layers

    def copy(src, dst, send, recv, to):
        return pltpu.make_async_remote_copy(
            src_ref=src, dst_ref=dst, send_sem=send, recv_sem=recv, device_id=to,
            device_id_type=pl.DeviceIdType.MESH,
        )

    def piece(u, slot):
        l, kind = divmod(u, 3)
        if kind < 2:
            depth = wv_hbm.shape[1]
            return wvg.at[2 * l + kind, pl.ds(pl.multiple_of(slot * depth, depth), depth)]
        depth = wo_hbm.shape[1]
        return wo.at[l, pl.ds(pl.multiple_of(slot * depth, depth), depth)]

    def lanes(u, yy):
        return u + sum(t < u for t in TWICE) + yy

    def sides(u):
        return (0, 1) if u in TWICE else (0,)

    def up_copy(u, yy, k):
        i, p = lanes(u, yy), piece(u, (z - k) * 2 + (1 - y if yy else y))
        return copy(p, p, su.at[i, k], ru.at[i, k], up)

    def down_copy(u, yy, k):
        i, p = lanes(u, yy), piece(u, (z + k) * 2 + (1 - y if yy else y))
        return copy(p, p, sd.at[i, k], rd.at[i, k], down)

    def beside_copy(u, oz):
        p = piece(u, oz * 2 + y)
        return copy(p, p, ys.at[u, oz], yr.at[u, oz], beside)

    def beside_wait(u, oz):
        p = piece(u, oz * 2 + 1 - y)
        copy(p, p, ys.at[u, oz], yr.at[u, oz], beside).wait_recv()

    def along(u, yy):
        pl.when(z + 1 < nz)(lambda: up_copy(u, yy, 0).start())
        pl.when(z > 0)(lambda: down_copy(u, yy, 0).start())

    def own(u):
        along(u, 0)
        beside_copy(u, z).start()

    def own_second(u):
        beside_wait(u, z)
        along(u, 1)

    def relay(u, d):
        for yy in sides(u):
            i = lanes(u, yy)
            side = 1 - y if yy else y

            @pl.when(z >= d)
            def _():
                p = piece(u, (z - d) * 2 + side)
                copy(p, p, su.at[i, d], ru.at[i, d - 1], beside).wait_recv()
                pl.when(z + 1 < nz)(lambda: up_copy(u, yy, d).start())
                if u not in TWICE:
                    beside_copy(u, z - d).start()

            @pl.when(z + d < nz)
            def _():
                p = piece(u, (z + d) * 2 + side)
                copy(p, p, sd.at[i, d], rd.at[i, d - 1], beside).wait_recv()
                pl.when(z > 0)(lambda: down_copy(u, yy, d).start())
                if u not in TWICE:
                    beside_copy(u, z + d).start()

    def arrive(u):
        if u not in TWICE:
            for oz in range(nz):
                beside_wait(u, oz)

    def sent():
        for u in range(units):
            for yy in sides(u):
                for k in range(nz - 1):
                    pl.when((z >= k) & (z + 1 < nz))(lambda: up_copy(u, yy, k).wait_send())
                    pl.when((z + k < nz) & (z > 0))(lambda: down_copy(u, yy, k).wait_send())
            if u in TWICE:
                beside_copy(u, z).wait_send()
            else:
                for oz in range(nz):
                    beside_copy(u, oz).wait_send()

    def gather(l):
        b = whole.at[l, tp]
        return (
            copy(b, b, gs.at[l, 0], gr.at[l, 0], mate),
            copy(b, b, gs.at[l, 1], gr.at[l, 1], across),
        )

    def gather_on(l):
        b = whole.at[l, (1 - x) * 2 + c]
        return copy(b, b, gs.at[l, 2], gr.at[l, 2], mate)

    def gather_wait(l):
        for j, t in ((0, x * 2 + 1 - c), (2, (1 - x) * 2 + 1 - c)):
            b = whole.at[l, t]
            copy(b, b, gs.at[l, j], gr.at[l, j], mate).wait_recv()

    def gather_start(l):
        for g in gather(l):
            g.start()

    def gather_turn(l):
        b = whole.at[l, (1 - x) * 2 + c]
        copy(b, b, gs.at[l, 1], gr.at[l, 1], across).wait_recv()
        gather_on(l).start()

    def norm(l):
        gather_wait(l)

        @pl.loop(0, rows // TILE)
        def _(i):
            r = pl.ds(pl.multiple_of(i * TILE, TILE), TILE)
            square = jnp.zeros((TILE, 1), jnp.float32)
            for t in range(ntp):
                v = whole[l, t, r, :].astype(jnp.float32)
                square = square + jnp.sum(v * v, -1, keepdims=True)
            scale = lax.rsqrt(square / (cols * ntp) + EPSILON)
            for t in range(ntp):
                v = whole[l, t, r, :].astype(jnp.float32)
                at = slice(t * cols, (t + 1) * cols)
                normed[r, at] = (v * scale * pre_ref[l : l + 1, at]).astype(jnp.bfloat16)

    def halo(l):
        to = lax.rem(sp + 1, nsp)
        return copy(
            glu.at[l, pl.ds(rows, HALO)], glu.at[l, pl.ds(0, HALO)], hs.at[l], hr.at[l], (to, tp)
        )

    def project(l):
        n = normed[...]
        for j in range(cols // 256):
            at = slice(j * 256, (j + 1) * 256)
            value = jnp.dot(n, wvg[2 * l, :, at], preferred_element_type=jnp.float32)
            gate = jnp.dot(n, wvg[2 * l + 1, :, at], preferred_element_type=jnp.float32)
            glu[l, HALO:, at] = (value * jax.nn.sigmoid(gate)).astype(jnp.bfloat16)
        pl.when(sp + 1 < nsp)(lambda: halo(l).start())

    def exchange(e):
        return [
            copy(stat.at[e], stat_in.at[e, j], ss.at[e, j], sr.at[e, j], to)
            for j, to in enumerate((mate, across, diagonal))
        ]

    def exchanged(e):
        for s in exchange(e):
            s.wait_recv()
        return stat[e] + stat_in[e, 0] + stat_in[e, 1] + stat_in[e, 2]

    lane = lax.broadcasted_iota(jnp.int32, (TILE, 128), 1)

    def pick(sums, at):
        return jnp.sum(jnp.where(lane == at, sums, 0.0), -1, keepdims=True)

    def convolve(l):
        @pl.when(sp == 0)
        def _():
            glu[l, :HALO] = jnp.zeros((HALO, cols), jnp.bfloat16)

        pl.when(sp > 0)(lambda: halo(l).wait_recv())
        first = HALO - (CONV_WIDTH - 1)

        def tile(i, sums):
            r = pl.multiple_of(i * TILE, TILE)
            one = jnp.zeros((TILE, 128), jnp.float32)
            two = jnp.zeros((TILE, 128), jnp.float32)
            for j in range(cols // 128):
                at = slice(j * 128, (j + 1) * 128)
                window = glu[l, pl.ds(r, TILE + HALO), at].astype(jnp.float32)
                acc = jnp.zeros((TILE, 128), jnp.float32)
                for s in range(8):
                    w = window if s == 0 else pltpu.roll(window, TILE + HALO - s, 0)
                    for k in range(CONV_WIDTH):
                        if (first + k) % 8 == s:
                            o = first + k - s
                            acc = acc + taps_ref[l, k : k + 1, at] * w[o : o + TILE]
                conv[pl.ds(r, TILE), at] = acc
                one = one + acc
                two = two + acc * acc
            sums = jnp.where(lane == 2 * i, jnp.sum(one, -1, keepdims=True), sums)
            return jnp.where(lane == 2 * i + 1, jnp.sum(two, -1, keepdims=True), sums)

        stat[2 * l] = lax.fori_loop(0, rows // TILE, tile, jnp.zeros((TILE, 128), jnp.float32))
        for s in exchange(2 * l):
            s.start()

    def activate(l):
        sums = exchanged(2 * l)

        @pl.loop(0, rows // TILE)
        def _(i):
            r = pl.ds(pl.multiple_of(i * TILE, TILE), TILE)
            center = pick(sums, 2 * i) / (cols * ntp)
            spread = jnp.maximum(pick(sums, 2 * i + 1) / (cols * ntp) - center * center, 0.0)
            v = (conv[r, :] - center) * lax.rsqrt(spread + LN_EPSILON)
            v = v * ng_ref[l : l + 1, :] + ns_ref[l : l + 1, :]
            act[r, :] = (v * jax.nn.sigmoid(v)).astype(jnp.bfloat16)

    each = wo_hbm.shape[2]
    per = cols // each
    depth = wo_hbm.shape[1]

    def term(l, t, h):
        w = wo[l, pl.ds(pl.multiple_of((t * per + h) * depth, depth), depth), :]
        return jnp.dot(act[...], w, preferred_element_type=jnp.float32).astype(jnp.bfloat16)

    def pair(l, far, h):
        i = far * per + h
        return copy(part_out.at[l, i], part_in.at[l, i], ps.at[l, i], pr.at[l, i], mate)

    def over(l, h):
        return copy(cross_out.at[l, h], cross_in.at[l, h], cs.at[l, h], cr.at[l, h], across)

    def give(l, far, h):
        t = ((1 - x) if far else x) * 2 + 1 - c
        part_out[l, far * per + h] = term(l, t, h)
        pair(l, far, h).start()

    def joined(l, far, h):
        t = ((1 - x) if far else x) * 2 + c
        mine = term(l, t, h).astype(jnp.float32)
        pair(l, far, h).wait_recv()
        return mine + part_in[l, far * per + h].astype(jnp.float32)

    def reduce(l):
        for h in range(per):
            give(l, 1, h)
        for h in range(per):
            cross_out[l, h] = joined(l, 1, h).astype(jnp.bfloat16)
            over(l, h).start()
        for h in range(per):
            give(l, 0, h)
        for h in range(per):
            total[:, h * each : (h + 1) * each] = joined(l, 0, h)

    def finish(l):
        for h in range(per):
            over(l, h).wait_recv()

        def tile(i, sums):
            r = pl.ds(pl.multiple_of(i * TILE, TILE), TILE)
            square = jnp.zeros((TILE, 1), jnp.float32)
            for h in range(per):
                at = slice(h * each, (h + 1) * each)
                p = total[r, at] + cross_in[l, h, r, :].astype(jnp.float32)
                p = p.astype(jnp.bfloat16).astype(jnp.float32)
                total[r, at] = p
                square = square + jnp.sum(p * p, -1, keepdims=True)
            return jnp.where(lane == i, square, sums)

        e = 2 * l + 1
        stat[e] = lax.fori_loop(0, rows // TILE, tile, jnp.zeros((TILE, 128), jnp.float32))
        for s in exchange(e):
            s.start()
        sums = exchanged(e)

        @pl.loop(0, rows // TILE)
        def _(i):
            r = pl.ds(pl.multiple_of(i * TILE, TILE), TILE)
            scale = lax.rsqrt(pick(sums, i) / (cols * ntp) + EPSILON)
            old = whole[l, tp, r, :].astype(jnp.float32)
            new = (old + total[r, :] * scale * post_ref[l : l + 1, :]).astype(jnp.bfloat16)
            if l + 1 < layers:
                whole[l + 1, tp, r, :] = new
            else:
                out_ref[r, :] = new

    held = [pltpu.make_async_copy(x_ref, whole.at[0, tp], local_sem.at[units])]
    for u in range(units):
        l, kind = divmod(u, 3)
        ref = (wv_hbm, wg_hbm, wo_hbm)[kind]
        held.append(pltpu.make_async_copy(ref.at[l], piece(u, sp), local_sem.at[u]))
    for h in held:
        h.start()
    barrier = pltpu.get_barrier_semaphore()
    for i in range(1, nsp):
        pl.semaphore_signal(
            barrier, inc=1, device_id=(lax.rem(sp + i, nsp), tp),
            device_id_type=pl.DeviceIdType.MESH,
        )
    for i in range(1, ntp):
        pl.semaphore_signal(
            barrier, inc=1, device_id=(sp, lax.rem(tp + i, ntp)),
            device_id_type=pl.DeviceIdType.MESH,
        )
    pl.semaphore_wait(barrier, nsp + ntp - 2)
    for h in held:
        h.wait()

    far = range(1, nz)
    gather_start(0)
    own(0)
    own(1)
    relay(0, 1)
    gather_turn(0)
    norm(0)
    for d in far[1:]:
        relay(0, d)
    own(2)
    for d in far:
        relay(1, d)
    own_second(2)
    own(3)
    arrive(0)
    relay(2, 1)
    arrive(1)
    project(0)
    relay(2, 2)
    convolve(0)
    for d in far[2:]:
        relay(2, d)
    activate(0)
    own(4)
    relay(3, 1)
    arrive(2)
    reduce(0)
    relay(3, 2)
    finish(0)
    gather_start(1)
    for d in far[2:]:
        relay(3, d)
    own(5)
    relay(4, 1)
    gather_turn(1)
    norm(1)
    for d in far[1:]:
        relay(4, d)
    arrive(3)
    relay(5, 1)
    arrive(4)
    project(1)
    relay(5, 2)
    convolve(1)
    for d in far[2:]:
        relay(5, d)
    activate(1)
    arrive(5)
    reduce(1)
    finish(1)

    sent()
    for l in range(layers):
        for g in (*gather(l), gather_on(l)):
            g.wait_send()
        pl.when(sp + 1 < nsp)(lambda: halo(l).wait_send())
        for s in (*exchange(2 * l), *exchange(2 * l + 1)):
            s.wait_send()
        for h in range(per):
            over(l, h).wait_send()
            for side in (0, 1):
                pair(l, side, h).wait_send()


def kernel_local(nsp, *args):
    tokens, pre_gain, w_value, _, _, _, _, w_out, _ = args
    rows, cols = tokens.shape
    layers, depth = w_value.shape[:2]
    inner, each = w_out.shape[1:]
    nz, units, per = nsp // 2, 3 * layers, cols // each
    tracks = units + len(TWICE)
    vmem, hbm = pl.BlockSpec(memory_space=pltpu.VMEM), pl.BlockSpec(memory_space=pl.ANY)
    bf16, f32, dma = jnp.bfloat16, jnp.float32, pltpu.SemaphoreType.DMA
    return pl.pallas_call(
        functools.partial(step, nz),
        out_shape=jax.ShapeDtypeStruct((rows, cols), bf16),
        in_specs=[hbm, vmem, hbm, hbm, vmem, vmem, vmem, hbm, vmem],
        out_specs=vmem,
        scratch_shapes=[
            pltpu.VMEM((2 * layers, nsp * depth, cols), bf16),
            pltpu.VMEM((layers, nsp * inner, each), bf16),
            pltpu.VMEM((layers, 4, rows, cols), bf16),
            pltpu.VMEM((rows, 4 * cols), bf16),
            pltpu.VMEM((layers, HALO + rows, cols), bf16),
            pltpu.VMEM((rows, cols), f32),
            pltpu.VMEM((rows, cols), bf16),
            pltpu.VMEM((layers, 2 * per, rows, each), bf16),
            pltpu.VMEM((layers, 2 * per, rows, each), bf16),
            pltpu.VMEM((layers, per, rows, each), bf16),
            pltpu.VMEM((layers, per, rows, each), bf16),
            pltpu.VMEM((rows, cols), f32),
            pltpu.VMEM((2 * layers, TILE, 128), f32),
            pltpu.VMEM((2 * layers, 3, TILE, 128), f32),
            dma((units + 1,)),
            dma((tracks, nz)), dma((tracks, nz)), dma((tracks, nz)), dma((tracks, nz)),
            dma((units, nz)), dma((units, nz)),
            dma((layers, 3)), dma((layers, 3)),
            dma((layers,)), dma((layers,)),
            dma((2 * layers, 3)), dma((2 * layers, 3)),
            dma((layers, 2 * per)), dma((layers, 2 * per)),
            dma((layers, per)), dma((layers, per)),
        ],
        compiler_params=pltpu.CompilerParams(
            collective_id=0, has_side_effects=True, vmem_limit_bytes=56 * 1024 * 1024
        ),
    )(*args)


def solution(mesh):
    nsp, ntp = mesh.shape["sp"], mesh.shape["tp"]
    fits = nsp % 2 == 0 and 3 <= nsp // 2 <= 8 and ntp == 4 and D // nsp % 128 == 0
    body = functools.partial(kernel_local, nsp) if fits else local
    placed = (
        P("sp", "tp"),
        P(),
        P(None, "sp", "tp"),
        P(None, "sp", "tp"),
        P(None, None, "tp"),
        P(None, "tp"),
        P(None, "tp"),
        P(None, "tp", "sp"),
        P(None, "tp"),
    )
    return jax.shard_map(
        body, mesh=mesh, in_specs=placed, out_specs=P("sp", "tp"), check_vma=False
    )
```

```python
import functools

import jax
import jax.numpy as jnp
from jax import lax
from jax.experimental import pallas as pl
from jax.experimental.pallas import tpu as pltpu
from jax.sharding import PartitionSpec as P

D = 2048
CONV_WIDTH = 31
LAYERS = 2


EPSILON = 1e-06
LN_EPSILON = 1e-05


def passed_along(block, axis, distance):
    devices = range(lax.axis_size(axis))
    route = [(i - distance, i) for i in devices if i - distance in devices]
    return lax.ppermute(block, axis, route)


def local(tokens, pre_gain, w_value, w_gate, taps, norm_gain, norm_shift, w_out, post_gain):
    stream = tokens
    full_value, full_gate = (
        lax.all_gather(w_value, "sp", axis=1, tiled=True),
        lax.all_gather(w_gate, "sp", axis=1, tiled=True),
    )
    full_out = lax.all_gather(w_out, "sp", axis=2, tiled=True)
    for layer in range(LAYERS):
        whole = lax.all_gather(stream, "tp", axis=1, tiled=True)
        whole_f = whole.astype(jnp.float32)
        normed = (
            whole_f
            * lax.rsqrt(jnp.mean(whole_f * whole_f, -1, keepdims=True) + EPSILON)
            * pre_gain[layer]
        ).astype(jnp.bfloat16)
        value_mat = full_value[layer]
        gate_mat = full_gate[layer]
        out_mat = full_out[layer]
        value_proj = jnp.dot(normed, value_mat, preferred_element_type=jnp.float32)
        gate_proj = jnp.dot(normed, gate_mat, preferred_element_type=jnp.float32)
        glu_act = (value_proj * jax.nn.sigmoid(gate_proj)).astype(jnp.bfloat16)
        rows = glu_act.shape[0]
        fringe = passed_along(glu_act[rows - (CONV_WIDTH - 1) :], "sp", 1)
        padded = jnp.concatenate([fringe, glu_act], 0).astype(jnp.float32)
        conv_out = jnp.zeros(glu_act.shape, jnp.float32)
        for offset in range(CONV_WIDTH):
            conv_out = conv_out + taps[layer, offset] * padded[offset : offset + rows]
        row_sum, row_square = lax.psum(
            (jnp.sum(conv_out, -1, keepdims=True), jnp.sum(conv_out * conv_out, -1, keepdims=True)),
            "tp",
        )
        center = row_sum / D
        spread = jnp.maximum(row_square / D - center * center, 0.0)
        activated = jax.nn.silu(
            (conv_out - center) * lax.rsqrt(spread + LN_EPSILON) * norm_gain[layer]
            + norm_shift[layer]
        ).astype(jnp.bfloat16)
        terms = jnp.dot(activated, out_mat, preferred_element_type=jnp.float32)
        summed = lax.psum_scatter(terms.astype(jnp.bfloat16), "tp", scatter_dimension=1, tiled=True)
        projected = summed.astype(jnp.float32)
        out_square = lax.psum(jnp.sum(projected * projected, -1, keepdims=True), "tp")
        scale = lax.rsqrt(out_square / D + EPSILON)
        stream = (stream.astype(jnp.float32) + projected * scale * post_gain[layer]).astype(
            jnp.bfloat16
        )
    return stream


TILE = 64
HALO = 32


def step(
    nz, x_ref, pre_ref, wv_hbm, wg_hbm, taps_ref, ng_ref, ns_ref, wo_hbm, post_ref, out_ref,
    wvg, other, wo, whole, normed, glu, conv, act, act_out, part_out, part_in, cross_out, cross_in,
    total, taps, gain, shift, stat, stat_in, local_sem,
    su, ru, sd, rd, ys, yr, gs, gr, hs, hr, ss, sr, ps, pr, cs, cr, acs, acr,
):
    sp, tp = lax.axis_index("sp"), lax.axis_index("tp")
    nsp, ntp = 2 * nz, 4
    z, y = sp // 2, sp % 2
    x, c = tp // 2, tp % 2
    up, down, beside = (sp + 2, tp), (sp - 2, tp), (z * 2 + 1 - y, tp)
    mate, across, diagonal = (sp, x * 2 + 1 - c), (sp, (1 - x) * 2 + c), (sp, (1 - x) * 2 + 1 - c)
    rows, cols = x_ref.shape
    layers = pre_ref.shape[0]
    units = 3 * layers
    both, half = 2 * rows, cols // 2
    twice = [u for u in range(units) if u % 3 < 2]
    mine = pl.ds(pl.multiple_of(y * half, half), half)

    def copy(src, dst, send, recv, to):
        return pltpu.make_async_remote_copy(
            src_ref=src, dst_ref=dst, send_sem=send, recv_sem=recv, device_id=to,
            device_id_type=pl.DeviceIdType.MESH,
        )

    def piece(u, slot):
        l, kind = divmod(u, 3)
        if kind < 2:
            depth = wv_hbm.shape[1]
            return wvg.at[2 * l + kind, pl.ds(pl.multiple_of(slot * depth, depth), depth)]
        depth = wo_hbm.shape[1]
        return wo.at[l, pl.ds(pl.multiple_of(slot * depth, depth), depth)]

    def lanes(u, yy):
        return u + sum(t < u for t in twice) + yy

    def sides(u):
        return (0, 1) if u in twice else (0,)

    def up_copy(u, yy, k):
        i, p = lanes(u, yy), piece(u, (z - k) * 2 + (1 - y if yy else y))
        return copy(p, p, su.at[i, k], ru.at[i, k], up)

    def down_copy(u, yy, k):
        i, p = lanes(u, yy), piece(u, (z + k) * 2 + (1 - y if yy else y))
        return copy(p, p, sd.at[i, k], rd.at[i, k], down)

    def beside_copy(u, oz):
        p = piece(u, oz * 2 + y)
        if u in twice:
            l, kind = divmod(u, 3)
            return copy(other.at[2 * l + kind], p, ys.at[u, oz], yr.at[u, oz], beside)
        return copy(p, p, ys.at[u, oz], yr.at[u, oz], beside)

    def beside_wait(u, oz):
        p = piece(u, oz * 2 + 1 - y)
        copy(p, p, ys.at[u, oz], yr.at[u, oz], beside).wait_recv()

    def along(u, yy):
        pl.when(z + 1 < nz)(lambda: up_copy(u, yy, 0).start())
        pl.when(z > 0)(lambda: down_copy(u, yy, 0).start())

    def own(u):
        along(u, 0)
        beside_copy(u, z).start()

    def own_second(u):
        beside_wait(u, z)
        along(u, 1)

    def relay(u, d):
        for yy in sides(u):
            i = lanes(u, yy)
            side = 1 - y if yy else y

            @pl.when(z >= d)
            def _():
                p = piece(u, (z - d) * 2 + side)
                copy(p, p, su.at[i, d], ru.at[i, d - 1], beside).wait_recv()
                pl.when(z + 1 < nz)(lambda: up_copy(u, yy, d).start())
                if u not in twice:
                    beside_copy(u, z - d).start()

            @pl.when(z + d < nz)
            def _():
                p = piece(u, (z + d) * 2 + side)
                copy(p, p, sd.at[i, d], rd.at[i, d - 1], beside).wait_recv()
                pl.when(z > 0)(lambda: down_copy(u, yy, d).start())
                if u not in twice:
                    beside_copy(u, z + d).start()

    def arrive(u):
        if u not in twice:
            for oz in range(nz):
                beside_wait(u, oz)

    def sent():
        for u in range(units):
            for yy in sides(u):
                for k in range(nz - 1):
                    pl.when((z >= k) & (z + 1 < nz))(lambda: up_copy(u, yy, k).wait_send())
                    pl.when((z + k < nz) & (z > 0))(lambda: down_copy(u, yy, k).wait_send())
            if u in twice:
                beside_copy(u, z).wait_send()
            else:
                for oz in range(nz):
                    beside_copy(u, oz).wait_send()

    here, there = y * 4, (1 - y) * 4
    opposite = (1 - x) * 2 + c

    routes = dict(
        across=(here + tp, across),
        beside=(here + tp, beside),
        mate=(here + tp, mate),
        across_mate=(here + opposite, mate),
        beside_across=(there + tp, across),
        beside_mate=(there + tp, mate),
        both_mate=(there + opposite, mate),
    )

    def gather(l, name):
        k = list(routes).index(name)
        t, to = routes[name]
        b = whole.at[l, t]
        return copy(b, b, gs.at[l, k], gr.at[l, k], to)

    def came(l, k, t):
        b = whole.at[l, t]
        copy(b, b, gs.at[l, k], gr.at[l, k], mate).wait_recv()

    def gather_start(l):
        for name in ("across", "beside", "mate"):
            gather(l, name).start()

    def gather_turn(l):
        came(l, 1, there + tp)
        gather(l, "beside_across").start()
        gather(l, "beside_mate").start()
        came(l, 0, here + opposite)
        gather(l, "across_mate").start()

    def gather_last(l):
        came(l, 4, there + opposite)
        gather(l, "both_mate").start()

    def gather_wait(l):
        pair_tp, pair_opposite = x * 2 + 1 - c, (1 - x) * 2 + 1 - c
        came(l, 2, here + pair_tp)
        came(l, 3, here + pair_opposite)
        came(l, 5, there + pair_tp)
        came(l, 6, there + pair_opposite)

    def norm(l):
        gather_wait(l)
        tiles = rows // TILE

        @pl.loop(0, 2 * tiles)
        def _(i):
            g, r = i // tiles * 4, pl.ds(pl.multiple_of(i % tiles * TILE, TILE), TILE)
            to = pl.ds(pl.multiple_of(i * TILE, TILE), TILE)
            square = jnp.zeros((TILE, 1), jnp.float32)
            for t in range(ntp):
                v = whole[l, g + t, r, :].astype(jnp.float32)
                square = square + jnp.sum(v * v, -1, keepdims=True)
            scale = lax.rsqrt(square / (cols * ntp) + EPSILON)
            for t in range(ntp):
                v = whole[l, g + t, r, :].astype(jnp.float32)
                at = slice(t * cols, (t + 1) * cols)
                normed[to, at] = (v * scale * pre_ref[l : l + 1, at]).astype(jnp.bfloat16)

    def halo(l):
        return copy(
            glu.at[l, pl.ds(both, HALO)], glu.at[l, pl.ds(0, HALO)], hs.at[l], hr.at[l], up
        )

    def project(l):
        n = normed[...]
        value = jnp.dot(n, wvg[2 * l], preferred_element_type=jnp.float32)
        gate = jnp.dot(n, wvg[2 * l + 1], preferred_element_type=jnp.float32)
        glu[l, HALO:, :] = (value * jax.nn.sigmoid(gate)).astype(jnp.bfloat16)
        pl.when(z + 1 < nz)(lambda: halo(l).start())

    partner = z * 2 + 1 - y
    peers = [mate, across, diagonal, beside]
    peers += [(partner, mate[1]), (partner, across[1]), (partner, diagonal[1])]

    def exchange(e):
        return [
            copy(stat.at[e], stat_in.at[e, j], ss.at[e, j], sr.at[e, j], to)
            for j, to in enumerate(peers[: 3 if e % 2 else 7])
        ]

    def exchanged(e):
        sums = stat[e]
        for j, s in enumerate(exchange(e)):
            s.wait_recv()
            sums = sums + stat_in[e, j]
        return sums

    lane = lax.broadcasted_iota(jnp.int32, (TILE, 128), 1)

    def pick(sums, at):
        return jnp.sum(jnp.where(lane == at, sums, 0.0), -1, keepdims=True)

    def convolve(l):
        @pl.when(z == 0)
        def _():
            glu[l, :HALO] = jnp.zeros((HALO, half), jnp.bfloat16)

        pl.when(z > 0)(lambda: halo(l).wait_recv())
        first = HALO - (CONV_WIDTH - 1)

        def tile(i, sums):
            r = pl.multiple_of(i * TILE, TILE)
            one = jnp.zeros((TILE, 128), jnp.float32)
            two = jnp.zeros((TILE, 128), jnp.float32)
            for j in range(half // 128):
                at = slice(j * 128, (j + 1) * 128)
                window = glu[l, pl.ds(r, TILE + HALO), at].astype(jnp.float32)
                acc = jnp.zeros((TILE, 128), jnp.float32)
                for s in range(8):
                    w = window if s == 0 else pltpu.roll(window, TILE + HALO - s, 0)
                    for k in range(CONV_WIDTH):
                        if (first + k) % 8 == s:
                            o = first + k - s
                            acc = acc + taps[l, k : k + 1, at] * w[o : o + TILE]
                conv[pl.ds(r, TILE), at] = acc
                one = one + acc
                two = two + acc * acc
            sums = jnp.where(lane == 2 * i, jnp.sum(one, -1, keepdims=True), sums)
            return jnp.where(lane == 2 * i + 1, jnp.sum(two, -1, keepdims=True), sums)

        stat[2 * l] = lax.fori_loop(0, both // TILE, tile, jnp.zeros((TILE, 128), jnp.float32))
        for s in exchange(2 * l):
            s.start()

    def activate(l):
        sums = exchanged(2 * l)
        tiles = rows // TILE

        def tile(q, i, store):
            at = q * tiles + i
            r = pl.ds(pl.multiple_of(at * TILE, TILE), TILE)
            center = pick(sums, 2 * at) / (cols * ntp)
            spread = jnp.maximum(pick(sums, 2 * at + 1) / (cols * ntp) - center * center, 0.0)
            v = (conv[r, :] - center) * lax.rsqrt(spread + LN_EPSILON)
            v = v * gain[l : l + 1, :] + shift[l : l + 1, :]
            store(pl.ds(pl.multiple_of(i * TILE, TILE), TILE), (v * jax.nn.sigmoid(v)).astype(jnp.bfloat16))

        def give_away(r, v):
            act_out[l, r, :] = v

        def keep(r, v):
            act[l, y, r, :] = v

        pl.loop(0, tiles)(lambda i: tile(1 - y, i, give_away))
        shared(l).start()
        pl.loop(0, tiles)(lambda i: tile(y, i, keep))
        b = act.at[l, 1 - y]
        copy(b, b, acs.at[l], acr.at[l], beside).wait_recv()

    def shared(l):
        return copy(act_out.at[l], act.at[l, y], acs.at[l], acr.at[l], beside)

    each = wo_hbm.shape[2]
    per = cols // each
    depth = wo_hbm.shape[1]

    def term(l, t, h):
        w = wo[l, pl.ds(pl.multiple_of((t * per + h) * depth, depth), depth), :]
        first = jnp.dot(act[l, 0], w[:half], preferred_element_type=jnp.float32)
        second = jnp.dot(act[l, 1], w[half:], preferred_element_type=jnp.float32)
        return (first + second).astype(jnp.bfloat16)

    def pair(l, far, h):
        i = far * per + h
        return copy(part_out.at[l, i], part_in.at[l, i], ps.at[l, i], pr.at[l, i], mate)

    def over(l, h):
        return copy(cross_out.at[l, h], cross_in.at[l, h], cs.at[l, h], cr.at[l, h], across)

    def give(l, far, h):
        t = ((1 - x) if far else x) * 2 + 1 - c
        part_out[l, far * per + h] = term(l, t, h)
        pair(l, far, h).start()

    def joined(l, far, h):
        t = ((1 - x) if far else x) * 2 + c
        kept = term(l, t, h).astype(jnp.float32)
        pair(l, far, h).wait_recv()
        return kept + part_in[l, far * per + h].astype(jnp.float32)

    def reduce(l):
        for h in range(per):
            give(l, 1, h)
        for h in range(per):
            cross_out[l, h] = joined(l, 1, h).astype(jnp.bfloat16)
            over(l, h).start()
        for h in range(per):
            give(l, 0, h)
        for h in range(per):
            total[:, h * each : (h + 1) * each] = joined(l, 0, h)

    def finish(l):
        for h in range(per):
            over(l, h).wait_recv()

        def tile(i, sums):
            r = pl.ds(pl.multiple_of(i * TILE, TILE), TILE)
            square = jnp.zeros((TILE, 1), jnp.float32)
            for h in range(per):
                at = slice(h * each, (h + 1) * each)
                p = total[r, at] + cross_in[l, h, r, :].astype(jnp.float32)
                p = p.astype(jnp.bfloat16).astype(jnp.float32)
                total[r, at] = p
                square = square + jnp.sum(p * p, -1, keepdims=True)
            return jnp.where(lane == i, square, sums)

        e = 2 * l + 1
        stat[e] = lax.fori_loop(0, rows // TILE, tile, jnp.zeros((TILE, 128), jnp.float32))
        for s in exchange(e):
            s.start()
        sums = exchanged(e)

        @pl.loop(0, rows // TILE)
        def _(i):
            r = pl.ds(pl.multiple_of(i * TILE, TILE), TILE)
            scale = lax.rsqrt(pick(sums, i) / (cols * ntp) + EPSILON)
            old = whole[l, here + tp, r, :].astype(jnp.float32)
            new = (old + total[r, :] * scale * post_ref[l : l + 1, :]).astype(jnp.bfloat16)
            if l + 1 < layers:
                whole[l + 1, here + tp, r, :] = new
            else:
                out_ref[r, :] = new

    held = [pltpu.make_async_copy(x_ref, whole.at[0, here + tp], local_sem.at[units])]
    for u in range(units):
        l, kind = divmod(u, 3)
        ref = (wv_hbm, wg_hbm, wo_hbm)[kind]
        if kind < 2:
            part = ref.at[l, :, mine]
            rest = ref.at[l, :, pl.ds(pl.multiple_of((1 - y) * half, half), half)]
            i = 2 * l + kind
            held.append(pltpu.make_async_copy(rest, other.at[i], local_sem.at[units + 1 + i]))
        else:
            part = ref.at[l]
        held.append(pltpu.make_async_copy(part, piece(u, sp), local_sem.at[u]))
    for h in held:
        h.start()
    for l in range(layers):
        taps[l] = taps_ref[l, :, mine]
        gain[l : l + 1] = ng_ref[l : l + 1, mine]
        shift[l : l + 1] = ns_ref[l : l + 1, mine]
    barrier = pltpu.get_barrier_semaphore()
    for i in range(1, nsp):
        pl.semaphore_signal(
            barrier, inc=1, device_id=(lax.rem(sp + i, nsp), tp),
            device_id_type=pl.DeviceIdType.MESH,
        )
    for i in range(1, ntp):
        for at in (sp, partner):
            pl.semaphore_signal(
                barrier, inc=1, device_id=(at, lax.rem(tp + i, ntp)),
                device_id_type=pl.DeviceIdType.MESH,
            )
    pl.semaphore_wait(barrier, nsp - 1 + 2 * (ntp - 1))
    for h in held:
        h.wait()

    far = range(1, nz)
    gather_start(0)
    own(0)
    own(1)
    own_second(0)
    own_second(1)
    relay(0, 1)
    gather_turn(0)
    for d in far[1:]:
        relay(0, d)
    gather_last(0)
    own(2)
    relay(1, 1)
    norm(0)
    for d in far[1:]:
        relay(1, d)
    own(3)
    own_second(3)
    relay(2, 1)
    project(0)
    relay(2, 2)
    convolve(0)
    for d in far[2:]:
        relay(2, d)
    own(4)
    own_second(4)
    relay(3, 1)
    activate(0)
    relay(3, 2)
    arrive(2)
    reduce(0)
    for d in far[2:]:
        relay(3, d)
    own(5)
    relay(4, 1)
    finish(0)
    gather_start(1)
    relay(4, 2)
    gather_turn(1)
    gather_last(1)
    for d in far[2:]:
        relay(4, d)
    norm(1)
    relay(5, 1)
    project(1)
    relay(5, 2)
    convolve(1)
    for d in far[2:]:
        relay(5, d)
    activate(1)
    arrive(5)
    reduce(1)
    finish(1)

    sent()
    for l in range(layers):
        for name in routes:
            gather(l, name).wait_send()
        pl.when(z + 1 < nz)(lambda: halo(l).wait_send())
        shared(l).wait_send()
        for s in (*exchange(2 * l), *exchange(2 * l + 1)):
            s.wait_send()
        for h in range(per):
            over(l, h).wait_send()
            for side in (0, 1):
                pair(l, side, h).wait_send()


def kernel_local(nsp, *args):
    tokens, pre_gain, w_value, _, _, _, _, w_out, _ = args
    rows, cols = tokens.shape
    layers, depth = w_value.shape[:2]
    inner, each = w_out.shape[1:]
    nz, units, per = nsp // 2, 3 * layers, cols // each
    tracks, half = units + 2 * layers, cols // 2
    vmem, hbm = pl.BlockSpec(memory_space=pltpu.VMEM), pl.BlockSpec(memory_space=pl.ANY)
    bf16, f32, dma = jnp.bfloat16, jnp.float32, pltpu.SemaphoreType.DMA
    return pl.pallas_call(
        functools.partial(step, nz),
        out_shape=jax.ShapeDtypeStruct((rows, cols), bf16),
        in_specs=[hbm, vmem, hbm, hbm, vmem, vmem, vmem, hbm, vmem],
        out_specs=vmem,
        scratch_shapes=[
            pltpu.VMEM((2 * layers, nsp * depth, half), bf16),
            pltpu.VMEM((2 * layers, depth, half), bf16),
            pltpu.VMEM((layers, nsp * inner, each), bf16),
            pltpu.VMEM((layers, 8, rows, cols), bf16),
            pltpu.VMEM((2 * rows, 4 * cols), bf16),
            pltpu.VMEM((layers, HALO + 2 * rows, half), bf16),
            pltpu.VMEM((2 * rows, half), f32),
            pltpu.VMEM((layers, 2, rows, half), bf16),
            pltpu.VMEM((layers, rows, half), bf16),
            pltpu.VMEM((layers, 2 * per, rows, each), bf16),
            pltpu.VMEM((layers, 2 * per, rows, each), bf16),
            pltpu.VMEM((layers, per, rows, each), bf16),
            pltpu.VMEM((layers, per, rows, each), bf16),
            pltpu.VMEM((rows, cols), f32),
            pltpu.VMEM((layers, CONV_WIDTH, half), f32),
            pltpu.VMEM((layers, half), f32),
            pltpu.VMEM((layers, half), f32),
            pltpu.VMEM((2 * layers, TILE, 128), f32),
            pltpu.VMEM((2 * layers, 7, TILE, 128), f32),
            dma((units + 1 + 2 * layers,)),
            dma((tracks, nz)), dma((tracks, nz)), dma((tracks, nz)), dma((tracks, nz)),
            dma((units, nz)), dma((units, nz)),
            dma((layers, 7)), dma((layers, 7)),
            dma((layers,)), dma((layers,)),
            dma((2 * layers, 7)), dma((2 * layers, 7)),
            dma((layers, 2 * per)), dma((layers, 2 * per)),
            dma((layers, per)), dma((layers, per)),
            dma((layers,)), dma((layers,)),
        ],
        compiler_params=pltpu.CompilerParams(
            collective_id=0, has_side_effects=True, vmem_limit_bytes=56 * 1024 * 1024
        ),
    )(*args)


def solution(mesh):
    nsp, ntp = mesh.shape["sp"], mesh.shape["tp"]
    fits = nsp % 2 == 0 and 3 <= nsp // 2 <= 8 and ntp == 4 and D // max(nsp, 2 * ntp) % 128 == 0
    body = functools.partial(kernel_local, nsp) if fits else local
    placed = (
        P("sp", "tp"),
        P(),
        P(None, "sp", "tp"),
        P(None, "sp", "tp"),
        P(None, None, "tp"),
        P(None, "tp"),
        P(None, "tp"),
        P(None, "tp", "sp"),
        P(None, "tp"),
    )
    return jax.shard_map(
        body, mesh=mesh, in_specs=placed, out_specs=P("sp", "tp"), check_vma=False
    )
```

```python
import functools

import jax
import jax.numpy as jnp
from jax import lax
from jax.experimental import pallas as pl
from jax.experimental.pallas import tpu as pltpu
from jax.sharding import PartitionSpec as P

D = 2048
CONV_WIDTH = 31
LAYERS = 2


EPSILON = 1e-06
LN_EPSILON = 1e-05


def passed_along(block, axis, distance):
    devices = range(lax.axis_size(axis))
    route = [(i - distance, i) for i in devices if i - distance in devices]
    return lax.ppermute(block, axis, route)


def local(tokens, pre_gain, w_value, w_gate, taps, norm_gain, norm_shift, w_out, post_gain):
    stream = tokens
    full_value, full_gate = (
        lax.all_gather(w_value, "sp", axis=1, tiled=True),
        lax.all_gather(w_gate, "sp", axis=1, tiled=True),
    )
    full_out = lax.all_gather(w_out, "sp", axis=2, tiled=True)
    for layer in range(LAYERS):
        whole = lax.all_gather(stream, "tp", axis=1, tiled=True)
        whole_f = whole.astype(jnp.float32)
        normed = (
            whole_f
            * lax.rsqrt(jnp.mean(whole_f * whole_f, -1, keepdims=True) + EPSILON)
            * pre_gain[layer]
        ).astype(jnp.bfloat16)
        value_mat = full_value[layer]
        gate_mat = full_gate[layer]
        out_mat = full_out[layer]
        value_proj = jnp.dot(normed, value_mat, preferred_element_type=jnp.float32)
        gate_proj = jnp.dot(normed, gate_mat, preferred_element_type=jnp.float32)
        glu_act = (value_proj * jax.nn.sigmoid(gate_proj)).astype(jnp.bfloat16)
        rows = glu_act.shape[0]
        fringe = passed_along(glu_act[rows - (CONV_WIDTH - 1) :], "sp", 1)
        padded = jnp.concatenate([fringe, glu_act], 0).astype(jnp.float32)
        conv_out = jnp.zeros(glu_act.shape, jnp.float32)
        for offset in range(CONV_WIDTH):
            conv_out = conv_out + taps[layer, offset] * padded[offset : offset + rows]
        row_sum, row_square = lax.psum(
            (jnp.sum(conv_out, -1, keepdims=True), jnp.sum(conv_out * conv_out, -1, keepdims=True)),
            "tp",
        )
        center = row_sum / D
        spread = jnp.maximum(row_square / D - center * center, 0.0)
        activated = jax.nn.silu(
            (conv_out - center) * lax.rsqrt(spread + LN_EPSILON) * norm_gain[layer]
            + norm_shift[layer]
        ).astype(jnp.bfloat16)
        terms = jnp.dot(activated, out_mat, preferred_element_type=jnp.float32)
        summed = lax.psum_scatter(terms.astype(jnp.bfloat16), "tp", scatter_dimension=1, tiled=True)
        projected = summed.astype(jnp.float32)
        out_square = lax.psum(jnp.sum(projected * projected, -1, keepdims=True), "tp")
        scale = lax.rsqrt(out_square / D + EPSILON)
        stream = (stream.astype(jnp.float32) + projected * scale * post_gain[layer]).astype(
            jnp.bfloat16
        )
    return stream


TILE = 64
PACK = 16
HALO = 32


def step(
    nz, x_ref, pre_ref, wv_hbm, wg_hbm, taps_ref, ng_ref, ns_ref, wo_hbm, post_ref, out_ref,
    wvg, other, wo, whole, normed, glu, conv, act, act_out, part_out, part_in, cross_out, cross_in,
    total, taps, gain, shift, stat, stat_in, local_sem,
    su, ru, sd, rd, ys, yr, gs, gr, hs, hr, ss, sr, ps, pr, cs, cr, acs, acr,
):
    sp, tp = lax.axis_index("sp"), lax.axis_index("tp")
    nsp, ntp = 2 * nz, 4
    z, y = sp // 2, sp % 2
    x, c = tp // 2, tp % 2
    up, down, beside = (sp + 2, tp), (sp - 2, tp), (z * 2 + 1 - y, tp)
    mate, across, diagonal = (sp, x * 2 + 1 - c), (sp, (1 - x) * 2 + c), (sp, (1 - x) * 2 + 1 - c)
    rows, cols = x_ref.shape
    layers = pre_ref.shape[0]
    units = 3 * layers
    both, half = 2 * rows, cols // 2
    twice = [u for u in range(units) if u % 3 < 2]
    mine = pl.ds(pl.multiple_of(y * half, half), half)

    def copy(src, dst, send, recv, to):
        return pltpu.make_async_remote_copy(
            src_ref=src, dst_ref=dst, send_sem=send, recv_sem=recv, device_id=to,
            device_id_type=pl.DeviceIdType.MESH,
        )

    def piece(u, slot):
        l, kind = divmod(u, 3)
        if kind < 2:
            depth = wv_hbm.shape[1]
            return wvg.at[2 * l + kind, pl.ds(pl.multiple_of(slot * depth, depth), depth)]
        depth = wo_hbm.shape[1]
        return wo.at[l, pl.ds(pl.multiple_of(slot * depth, depth), depth)]

    def lanes(u, yy):
        return u + sum(t < u for t in twice) + yy

    def sides(u):
        return (0, 1) if u in twice else (0,)

    def up_copy(u, yy, k):
        i, p = lanes(u, yy), piece(u, (z - k) * 2 + (1 - y if yy else y))
        return copy(p, p, su.at[i, k], ru.at[i, k], up)

    def down_copy(u, yy, k):
        i, p = lanes(u, yy), piece(u, (z + k) * 2 + (1 - y if yy else y))
        return copy(p, p, sd.at[i, k], rd.at[i, k], down)

    def beside_copy(u, oz):
        p = piece(u, oz * 2 + y)
        if u in twice:
            l, kind = divmod(u, 3)
            return copy(other.at[2 * l + kind], p, ys.at[u, oz], yr.at[u, oz], beside)
        return copy(p, p, ys.at[u, oz], yr.at[u, oz], beside)

    def beside_wait(u, oz):
        p = piece(u, oz * 2 + 1 - y)
        copy(p, p, ys.at[u, oz], yr.at[u, oz], beside).wait_recv()

    def along(u, yy):
        pl.when(z + 1 < nz)(lambda: up_copy(u, yy, 0).start())
        pl.when(z > 0)(lambda: down_copy(u, yy, 0).start())

    def own(u):
        along(u, 0)
        beside_copy(u, z).start()

    def own_second(u):
        beside_wait(u, z)
        along(u, 1)

    def relay(u, d):
        for yy in sides(u):
            i = lanes(u, yy)
            side = 1 - y if yy else y

            @pl.when(z >= d)
            def _():
                p = piece(u, (z - d) * 2 + side)
                copy(p, p, su.at[i, d], ru.at[i, d - 1], beside).wait_recv()
                pl.when(z + 1 < nz)(lambda: up_copy(u, yy, d).start())
                if u not in twice:
                    beside_copy(u, z - d).start()

            @pl.when(z + d < nz)
            def _():
                p = piece(u, (z + d) * 2 + side)
                copy(p, p, sd.at[i, d], rd.at[i, d - 1], beside).wait_recv()
                pl.when(z > 0)(lambda: down_copy(u, yy, d).start())
                if u not in twice:
                    beside_copy(u, z + d).start()

    def arrive(u):
        if u not in twice:
            for oz in range(nz):
                beside_wait(u, oz)

    def sent():
        for u in range(units):
            for yy in sides(u):
                for k in range(nz - 1):
                    pl.when((z >= k) & (z + 1 < nz))(lambda: up_copy(u, yy, k).wait_send())
                    pl.when((z + k < nz) & (z > 0))(lambda: down_copy(u, yy, k).wait_send())
            if u in twice:
                beside_copy(u, z).wait_send()
            else:
                for oz in range(nz):
                    beside_copy(u, oz).wait_send()

    here, there = y * 4, (1 - y) * 4
    opposite = (1 - x) * 2 + c

    routes = dict(
        across=(here + tp, across),
        beside=(here + tp, beside),
        mate=(here + tp, mate),
        across_mate=(here + opposite, mate),
        beside_across=(there + tp, across),
        beside_mate=(there + tp, mate),
        both_mate=(there + opposite, mate),
        across_beside=(here + opposite, beside),
    )
    upper, lower = pl.ds(0, rows // 2), pl.ds(rows // 2, rows // 2)
    parts = dict(beside_across=upper, across_beside=lower)

    def gather(l, name):
        k = list(routes).index(name)
        t, to = routes[name]
        b = whole.at[l, t, parts[name]] if name in parts else whole.at[l, t]
        return copy(b, b, gs.at[l, k], gr.at[l, k], to)

    def came(l, k, t, part=pl.ds(0, rows)):
        b = whole.at[l, t, part]
        copy(b, b, gs.at[l, k], gr.at[l, k], mate).wait_recv()

    def gather_start(l):
        for name in ("across", "beside", "mate"):
            gather(l, name).start()

    def gather_turn(l):
        came(l, 1, there + tp)
        gather(l, "beside_across").start()
        gather(l, "beside_mate").start()
        came(l, 0, here + opposite)
        gather(l, "across_beside").start()
        gather(l, "across_mate").start()

    def gather_last(l):
        came(l, 4, there + opposite, upper)
        came(l, 7, there + opposite, lower)
        gather(l, "both_mate").start()

    def gather_wait(l):
        pair_tp, pair_opposite = x * 2 + 1 - c, (1 - x) * 2 + 1 - c
        came(l, 2, here + pair_tp)
        came(l, 3, here + pair_opposite)
        came(l, 5, there + pair_tp)
        came(l, 6, there + pair_opposite)

    def norm(l):
        gather_wait(l)
        tiles = rows // TILE

        @pl.loop(0, 2 * tiles)
        def _(i):
            g, r = i // tiles * 4, pl.ds(pl.multiple_of(i % tiles * TILE, TILE), TILE)
            to = pl.ds(pl.multiple_of(i * TILE, TILE), TILE)
            square = jnp.zeros((TILE, 1), jnp.float32)
            for t in range(ntp):
                v = whole[l, g + t, r, :].astype(jnp.float32)
                square = square + jnp.sum(v * v, -1, keepdims=True)
            scale = lax.rsqrt(square / (cols * ntp) + EPSILON)
            for t in range(ntp):
                v = whole[l, g + t, r, :].astype(jnp.float32)
                at = slice(t * cols, (t + 1) * cols)
                normed[to, at] = (v * scale * pre_ref[l : l + 1, at]).astype(jnp.bfloat16)

    def halo(l):
        return copy(
            glu.at[l, pl.ds(both, HALO)], glu.at[l, pl.ds(0, HALO)], hs.at[l], hr.at[l], up
        )

    def project(l):
        n = normed[...]
        value = jnp.dot(n, wvg[2 * l], preferred_element_type=jnp.float32)
        gate = jnp.dot(n, wvg[2 * l + 1], preferred_element_type=jnp.float32)
        glu[l, HALO:, :] = (value * jax.nn.sigmoid(gate)).astype(jnp.bfloat16)
        pl.when(z + 1 < nz)(lambda: halo(l).start())

    partner = z * 2 + 1 - y
    peers = [mate, across, diagonal, beside]
    peers += [(partner, mate[1]), (partner, across[1]), (partner, diagonal[1])]

    def exchange(e):
        return [
            copy(stat.at[e], stat_in.at[e, j], ss.at[e, j], sr.at[e, j], to)
            for j, to in enumerate(peers[: 3 if e % 2 else 7])
        ]

    def exchanged(e):
        sums = stat[e]
        for j, s in enumerate(exchange(e)):
            s.wait_recv()
            sums = sums + stat_in[e, j]
        return sums

    lane = lax.broadcasted_iota(jnp.int32, (PACK, 128), 1)
    groups = TILE // PACK

    def pick(sums, at):
        found = [
            jnp.sum(jnp.where(lane == at * groups + g, sums, 0.0), -1, keepdims=True)
            for g in range(groups)
        ]
        return jnp.concatenate(found, 0)

    def pack(sums, at, column):
        for g in range(groups):
            sums = jnp.where(lane == at * groups + g, column[g * PACK : (g + 1) * PACK], sums)
        return sums

    def convolve(l):
        @pl.when(z == 0)
        def _():
            glu[l, :HALO] = jnp.zeros((HALO, half), jnp.bfloat16)

        pl.when(z > 0)(lambda: halo(l).wait_recv())
        first = HALO - (CONV_WIDTH - 1)

        def tile(i, sums):
            r = pl.multiple_of(i * TILE, TILE)
            one = jnp.zeros((TILE, 128), jnp.float32)
            two = jnp.zeros((TILE, 128), jnp.float32)
            for j in range(half // 128):
                at = slice(j * 128, (j + 1) * 128)
                window = glu[l, pl.ds(r, TILE + HALO), at].astype(jnp.float32)
                acc = jnp.zeros((TILE, 128), jnp.float32)
                for s in range(8):
                    w = window if s == 0 else pltpu.roll(window, TILE + HALO - s, 0)
                    for k in range(CONV_WIDTH):
                        if (first + k) % 8 == s:
                            o = first + k - s
                            acc = acc + taps[l, k : k + 1, at] * w[o : o + TILE]
                conv[pl.ds(r, TILE), at] = acc
                one = one + acc
                two = two + acc * acc
            sums = pack(sums, 2 * i, jnp.sum(one, -1, keepdims=True))
            return pack(sums, 2 * i + 1, jnp.sum(two, -1, keepdims=True))

        stat[2 * l] = lax.fori_loop(0, both // TILE, tile, jnp.zeros((PACK, 128), jnp.float32))
        for s in exchange(2 * l):
            s.start()

    def activate(l):
        sums = exchanged(2 * l)
        tiles = rows // TILE

        def tile(q, i, store):
            at = q * tiles + i
            r = pl.ds(pl.multiple_of(at * TILE, TILE), TILE)
            center = pick(sums, 2 * at) / (cols * ntp)
            spread = jnp.maximum(pick(sums, 2 * at + 1) / (cols * ntp) - center * center, 0.0)
            v = (conv[r, :] - center) * lax.rsqrt(spread + LN_EPSILON)
            v = v * gain[l : l + 1, :] + shift[l : l + 1, :]
            store(pl.ds(pl.multiple_of(i * TILE, TILE), TILE), (v * jax.nn.sigmoid(v)).astype(jnp.bfloat16))

        def give_away(r, v):
            act_out[l, r, :] = v

        def keep(r, v):
            act[l, y, r, :] = v

        pl.loop(0, tiles)(lambda i: tile(1 - y, i, give_away))
        shared(l).start()
        pl.loop(0, tiles)(lambda i: tile(y, i, keep))
        b = act.at[l, 1 - y]
        copy(b, b, acs.at[l], acr.at[l], beside).wait_recv()

    def shared(l):
        return copy(act_out.at[l], act.at[l, y], acs.at[l], acr.at[l], beside)

    each = wo_hbm.shape[2]
    per = cols // each
    depth = wo_hbm.shape[1]

    def term(l, t, h):
        w = wo[l, pl.ds(pl.multiple_of((t * per + h) * depth, depth), depth), :]
        first = jnp.dot(act[l, 0], w[:half], preferred_element_type=jnp.float32)
        second = jnp.dot(act[l, 1], w[half:], preferred_element_type=jnp.float32)
        return (first + second).astype(jnp.bfloat16)

    def pair(l, far, h):
        i = far * per + h
        return copy(part_out.at[l, i], part_in.at[l, i], ps.at[l, i], pr.at[l, i], mate)

    def over(l, h):
        return copy(cross_out.at[l, h], cross_in.at[l, h], cs.at[l, h], cr.at[l, h], across)

    def give(l, far, h):
        t = ((1 - x) if far else x) * 2 + 1 - c
        part_out[l, far * per + h] = term(l, t, h)
        pair(l, far, h).start()

    def joined(l, far, h):
        t = ((1 - x) if far else x) * 2 + c
        kept = term(l, t, h).astype(jnp.float32)
        pair(l, far, h).wait_recv()
        return kept + part_in[l, far * per + h].astype(jnp.float32)

    def reduce(l):
        for h in range(per):
            give(l, 1, h)
        for h in range(per):
            cross_out[l, h] = joined(l, 1, h).astype(jnp.bfloat16)
            over(l, h).start()
        for h in range(per):
            give(l, 0, h)
        for h in range(per):
            total[:, h * each : (h + 1) * each] = joined(l, 0, h)

    def finish(l):
        for h in range(per):
            over(l, h).wait_recv()

        def tile(i, sums):
            r = pl.ds(pl.multiple_of(i * TILE, TILE), TILE)
            square = jnp.zeros((TILE, 1), jnp.float32)
            for h in range(per):
                at = slice(h * each, (h + 1) * each)
                p = total[r, at] + cross_in[l, h, r, :].astype(jnp.float32)
                p = p.astype(jnp.bfloat16).astype(jnp.float32)
                total[r, at] = p
                square = square + jnp.sum(p * p, -1, keepdims=True)
            return pack(sums, i, square)

        e = 2 * l + 1
        stat[e] = lax.fori_loop(0, rows // TILE, tile, jnp.zeros((PACK, 128), jnp.float32))
        for s in exchange(e):
            s.start()
        sums = exchanged(e)

        @pl.loop(0, rows // TILE)
        def _(i):
            r = pl.ds(pl.multiple_of(i * TILE, TILE), TILE)
            scale = lax.rsqrt(pick(sums, i) / (cols * ntp) + EPSILON)
            old = whole[l, here + tp, r, :].astype(jnp.float32)
            new = (old + total[r, :] * scale * post_ref[l : l + 1, :]).astype(jnp.bfloat16)
            if l + 1 < layers:
                whole[l + 1, here + tp, r, :] = new
            else:
                out_ref[r, :] = new

    held = [pltpu.make_async_copy(x_ref, whole.at[0, here + tp], local_sem.at[units])]
    for u in range(units):
        l, kind = divmod(u, 3)
        ref = (wv_hbm, wg_hbm, wo_hbm)[kind]
        if kind < 2:
            part = ref.at[l, :, mine]
            rest = ref.at[l, :, pl.ds(pl.multiple_of((1 - y) * half, half), half)]
            i = 2 * l + kind
            held.append(pltpu.make_async_copy(rest, other.at[i], local_sem.at[units + 1 + i]))
        else:
            part = ref.at[l]
        held.append(pltpu.make_async_copy(part, piece(u, sp), local_sem.at[u]))
    for h in held:
        h.start()
    for l in range(layers):
        taps[l] = taps_ref[l, :, mine]
        gain[l : l + 1] = ng_ref[l : l + 1, mine]
        shift[l : l + 1] = ns_ref[l : l + 1, mine]
    barrier = pltpu.get_barrier_semaphore()
    for i in range(1, nsp):
        pl.semaphore_signal(
            barrier, inc=1, device_id=(lax.rem(sp + i, nsp), tp),
            device_id_type=pl.DeviceIdType.MESH,
        )
    for i in range(1, ntp):
        for at in (sp, partner):
            pl.semaphore_signal(
                barrier, inc=1, device_id=(at, lax.rem(tp + i, ntp)),
                device_id_type=pl.DeviceIdType.MESH,
            )
    pl.semaphore_wait(barrier, nsp - 1 + 2 * (ntp - 1))
    for h in held:
        h.wait()

    far = range(1, nz)
    gather_start(0)
    own(0)
    own(1)
    own_second(0)
    own_second(1)
    relay(0, 1)
    gather_turn(0)
    for d in far[1:]:
        relay(0, d)
    gather_last(0)
    own(2)
    relay(1, 1)
    norm(0)
    for d in far[1:]:
        relay(1, d)
    own(3)
    own_second(3)
    project(0)
    relay(2, 1)
    convolve(0)
    relay(2, 2)
    activate(0)
    for d in far[2:]:
        relay(2, d)
    own(4)
    own_second(4)
    relay(3, 1)
    arrive(2)
    reduce(0)
    relay(3, 2)
    for d in far[2:]:
        relay(3, d)
    own(5)
    finish(0)
    gather_start(1)
    relay(4, 1)
    gather_turn(1)
    relay(4, 2)
    for d in far[2:]:
        relay(4, d)
    gather_last(1)
    relay(5, 1)
    norm(1)
    project(1)
    relay(5, 2)
    convolve(1)
    for d in far[2:]:
        relay(5, d)
    activate(1)
    arrive(5)
    reduce(1)
    finish(1)

    sent()
    for l in range(layers):
        for name in routes:
            gather(l, name).wait_send()
        pl.when(z + 1 < nz)(lambda: halo(l).wait_send())
        shared(l).wait_send()
        for s in (*exchange(2 * l), *exchange(2 * l + 1)):
            s.wait_send()
        for h in range(per):
            over(l, h).wait_send()
            for side in (0, 1):
                pair(l, side, h).wait_send()


def kernel_local(nsp, *args):
    tokens, pre_gain, w_value, _, _, _, _, w_out, _ = args
    rows, cols = tokens.shape
    if rows % TILE or 4 * rows > PACK * 128:
        return local(*args)
    layers, depth = w_value.shape[:2]
    inner, each = w_out.shape[1:]
    nz, units, per = nsp // 2, 3 * layers, cols // each
    tracks, half = units + 2 * layers, cols // 2
    vmem, hbm = pl.BlockSpec(memory_space=pltpu.VMEM), pl.BlockSpec(memory_space=pl.ANY)
    bf16, f32, dma = jnp.bfloat16, jnp.float32, pltpu.SemaphoreType.DMA
    return pl.pallas_call(
        functools.partial(step, nz),
        out_shape=jax.ShapeDtypeStruct((rows, cols), bf16),
        in_specs=[hbm, vmem, hbm, hbm, vmem, vmem, vmem, hbm, vmem],
        out_specs=vmem,
        scratch_shapes=[
            pltpu.VMEM((2 * layers, nsp * depth, half), bf16),
            pltpu.VMEM((2 * layers, depth, half), bf16),
            pltpu.VMEM((layers, nsp * inner, each), bf16),
            pltpu.VMEM((layers, 8, rows, cols), bf16),
            pltpu.VMEM((2 * rows, 4 * cols), bf16),
            pltpu.VMEM((layers, HALO + 2 * rows, half), bf16),
            pltpu.VMEM((2 * rows, half), f32),
            pltpu.VMEM((layers, 2, rows, half), bf16),
            pltpu.VMEM((layers, rows, half), bf16),
            pltpu.VMEM((layers, 2 * per, rows, each), bf16),
            pltpu.VMEM((layers, 2 * per, rows, each), bf16),
            pltpu.VMEM((layers, per, rows, each), bf16),
            pltpu.VMEM((layers, per, rows, each), bf16),
            pltpu.VMEM((rows, cols), f32),
            pltpu.VMEM((layers, CONV_WIDTH, half), f32),
            pltpu.VMEM((layers, half), f32),
            pltpu.VMEM((layers, half), f32),
            pltpu.VMEM((2 * layers, PACK, 128), f32),
            pltpu.VMEM((2 * layers, 7, PACK, 128), f32),
            dma((units + 1 + 2 * layers,)),
            dma((tracks, nz)), dma((tracks, nz)), dma((tracks, nz)), dma((tracks, nz)),
            dma((units, nz)), dma((units, nz)),
            dma((layers, 8)), dma((layers, 8)),
            dma((layers,)), dma((layers,)),
            dma((2 * layers, 7)), dma((2 * layers, 7)),
            dma((layers, 2 * per)), dma((layers, 2 * per)),
            dma((layers, per)), dma((layers, per)),
            dma((layers,)), dma((layers,)),
        ],
        compiler_params=pltpu.CompilerParams(
            collective_id=0, has_side_effects=True, vmem_limit_bytes=56 * 1024 * 1024
        ),
    )(*args)


def solution(mesh):
    nsp, ntp = mesh.shape["sp"], mesh.shape["tp"]
    fits = nsp % 2 == 0 and 3 <= nsp // 2 <= 8 and ntp == 4 and D // max(nsp, 2 * ntp) % 128 == 0
    body = functools.partial(kernel_local, nsp) if fits else local
    placed = (
        P("sp", "tp"),
        P(),
        P(None, "sp", "tp"),
        P(None, "sp", "tp"),
        P(None, None, "tp"),
        P(None, "tp"),
        P(None, "tp"),
        P(None, "tp", "sp"),
        P(None, "tp"),
    )
    return jax.shard_map(
        body, mesh=mesh, in_specs=placed, out_specs=P("sp", "tp"), check_vma=False
    )
```
